32 devices in a mesh: fs: 8 (over z, y), tp: 4 (over x, core).
Axes of the slice: x: 2, y: 2, z: 4, core: 2. Of those that a mesh axis runs over, the one named last changes fastest.
Arguments:
- fresh_rows: bfloat16 [4096, 2048], P('fs'), may hold values from -6 to 6
- saved_rows: bfloat16 [4096, 2048], P('fs'), may hold values from -6 to 6
- upstream_grad: bfloat16 [4096, 2048], P('fs'), may hold values from -6 to 6
- proj_up: bfloat16 [2048, 8192], P('fs', 'tp'), may hold values from -0.125 to 0.125
- proj_down: bfloat16 [2048, 8192], P('fs', 'tp'), may hold values from -0.0625 to 0.0625
- accum_up: float32 [2048, 8192], P('fs', 'tp'), may hold values from -6 to 6
- accum_down: float32 [2048, 8192], P('fs', 'tp'), may hold values from -6 to 6
Outputs:
- fresh_out: bfloat16 [4096, 2048], P(('fs', 'tp'))
- saved_grad: bfloat16 [4096, 2048], P(('fs', 'tp'))
- accum_up_out: float32 [2048, 8192], P('fs', 'tp')
- accum_down_out: float32 [2048, 8192], P('fs', 'tp')
The draws below stay inside these ranges and needn't reach their ends.
All inputs are finite; a program needn't handle non-finite values.
Results may differ from the reference program's by a relative error of at most 0.014.
Values may be sent and summed in bfloat16 or wider, within the bound.
A program may use at most 128 MiB of HBM per device.

```python
import jax
import jax.numpy as jnp
from jax import lax

D = 2048
FF = 8192
TOKENS = 4096
N_TP = 4


def raised(result, stream_key, source, target, shards_of, factor):
    owner, partner = [(jnp.arange(result.shape[axis_at]) // (result.shape[axis_at] // shards_of)).reshape([-1 if axis == axis_at else 1 for axis in range(result.ndim)]) for axis_at in (source, target)]
    chosen = jax.random.permutation(stream_key, shards_of)[partner]
    strong = (owner == chosen) | (owner == (partner + shards_of // 2) % shards_of)
    return jnp.where(strong, factor * result, result)


def block_levels(key, dims, split, least, top_value):
    factor_of = 1.0
    for axis_at, parts in split:
        draws = jax.random.uniform(jax.random.fold_in(jax.random.fold_in(key, 6), axis_at), (parts,), jnp.float32, least / len(split), top_value / len(split))
        factor_of = factor_of * jnp.repeat(jnp.exp(draws), dims[axis_at] // parts).reshape((-1,) + (1,) * (len(dims) - 1 - axis_at))
    return factor_of


def gaussian(stream_key, extent, spread, reach, shards=(), held_as=jnp.bfloat16):
    level = block_levels(stream_key, extent, shards, -0.22, 0.18) if shards else 1.0
    values = jax.random.normal(stream_key, extent, jnp.float32) * spread * level
    return jnp.minimum(jnp.maximum(values, -reach), reach).astype(held_as)


def heavy_noise(rng, dims, spread, bound, cuts, heavy, held_as=jnp.bfloat16):
    drawn = spread * jax.random.normal(rng, dims, jnp.float32)
    if cuts:
        drawn = drawn * block_levels(rng, dims, cuts, -0.22, 0.18)
    return jnp.clip(raised(drawn, jax.random.fold_in(rng, 3), *heavy), -bound, bound).astype(held_as)


def setup_inputs(seed: int = 0) -> dict:
    splits = jax.random.split(jax.random.key(seed), 8)
    return {
        "fresh_rows": gaussian(splits[0], (TOKENS, D), 1.0, 6.0, ((0, 8),)),
        "saved_rows": gaussian(splits[1], (TOKENS, D), 1.0, 6.0, ((0, 8),)),
        "upstream_grad": heavy_noise(splits[2], (TOKENS, D), 1.0, 6.0, ((0, 8),), (0, 1, 8, 2.0)),
        "proj_up": gaussian(splits[3], (D, FF), D ** -0.5, 0.125, ((0, 8), (1, 4))),
        "proj_down": gaussian(splits[4], (D, FF), FF ** -0.5, 0.0625, ((0, 8), (1, 4))),
        "accum_up": gaussian(splits[5], (D, FF), 1.0, 6.0, ((0, 8), (1, 4)), jnp.float32),
        "accum_down": gaussian(splits[6], (D, FF), 1.0, 6.0, ((0, 8), (1, 4)), jnp.float32),
    }


def block_sum(left, right):
    width = FF // N_TP

    def add_block(index, running):
        first = (index * width).astype(jnp.int32)
        left_part = lax.dynamic_slice_in_dim(left, first, width, 1)
        right_part = lax.dynamic_slice_in_dim(right, first, width, 1)
        partial_sum = jnp.dot(left_part, right_part.T, preferred_element_type=jnp.float32)
        rounded = lax.optimization_barrier(partial_sum.astype(jnp.bfloat16))
        return running + rounded.astype(jnp.float32)

    empty = jnp.zeros((left.shape[0], right.shape[0]), jnp.float32)
    return lax.fori_loop(0, N_TP, add_block, empty).astype(jnp.bfloat16)


def reference(fresh_rows, saved_rows, upstream_grad, proj_up, proj_down, accum_up, accum_down):
    grad_scale = float(TOKENS) ** -0.5
    fresh_pre = jnp.dot(fresh_rows, proj_up, preferred_element_type=jnp.float32)
    fresh_active = jnp.maximum(fresh_pre, 0.0)
    fresh_hidden = (fresh_active * fresh_active).astype(jnp.bfloat16)
    fresh_out = block_sum(fresh_hidden, proj_down)
    saved_pre = jnp.dot(saved_rows, proj_up, preferred_element_type=jnp.float32)
    saved_active = jnp.maximum(saved_pre, 0.0)
    saved_hidden = (saved_active * saved_active).astype(jnp.bfloat16)
    hidden_grad = jnp.dot(upstream_grad, proj_down, preferred_element_type=jnp.float32)
    pre_grad = (2.0 * saved_active * hidden_grad).astype(jnp.bfloat16)
    saved_grad = block_sum(pre_grad, proj_up)
    up_term = jnp.dot(saved_rows.T, pre_grad, preferred_element_type=jnp.float32)
    down_term = jnp.dot(upstream_grad.T, saved_hidden, preferred_element_type=jnp.float32)
    accum_up_out = accum_up + grad_scale * up_term
    accum_down_out = accum_down + grad_scale * down_term
    return fresh_out, saved_grad, accum_up_out, accum_down_out
```

```python
import jax
import jax.numpy as jnp
from jax import lax
from jax.sharding import PartitionSpec as P


BF = jnp.bfloat16
F32 = jnp.float32


def against_rows(left, right):
    return lax.dot_general(left, right, (((1,), (1,)), ((), ())), preferred_element_type=F32)


def over_tokens(left, right):
    return lax.dot_general(left, right, (((0,), (0,)), ((), ())), preferred_element_type=F32)


def squared_relu(pre_values):
    active = jnp.maximum(pre_values, 0.0)
    return (active, (active * active).astype(BF))


def body(fresh_rows, saved_rows, upstream_grad, proj_up, proj_down, accum_up, accum_down):
    fs_n, tp_n = lax.axis_size("fs"), lax.axis_size("tp")
    line_n = fs_n // 2
    fs, tp = lax.axis_index("fs"), lax.axis_index("tp")
    line, side = fs // 2, fs % 2
    row_count, width = fresh_rows.shape
    depth, columns = proj_up.shape
    half = columns // 2
    grad_scale = float(row_count * fs_n) ** (-0.5)

    def to_side(value):
        return lax.ppermute(value, "fs", [(i, i ^ 1) for i in range(fs_n)])

    def to_tp(value, bit):
        return lax.ppermute(value, "tp", [(j, j ^ bit) for j in range(tp_n)])

    def along(value, lines, way):
        return lax.ppermute(
            value,
            "fs",
            [(l * 2 + s, (l + way) * 2 + s) for l in lines for s in range(2)],
        )

    def side_block(weight):
        mine = lax.dynamic_slice_in_dim(weight, side * half, half, 1)
        other = lax.dynamic_slice_in_dim(weight, (1 - side) * half, half, 1)
        return jnp.concatenate((mine, to_side(other)), axis=0)

    def line_gather(block):
        ups, downs = [block], [block]
        for step in range(1, line_n):
            ups.append(along(ups[-1], range(step - 1, line_n - 1), 1))
            downs.append(along(downs[-1], range(1, line_n - step + 1), -1))
        blocks = [block] + [
            jnp.where(line >= k, ups[k], downs[line_n - k]) for k in range(1, line_n)
        ]
        return jnp.concatenate(blocks, axis=0), (ups[-1], downs[-1])

    def line_sum(grads):
        size = 2 * depth
        up = down = None
        for step in range(1, line_n):
            low = grads[step * size : (step + 1) * size]
            high = grads[(line_n - step) * size : (line_n - step + 1) * size]
            low = low if up is None else low + up.astype(F32)
            high = high if down is None else high + down.astype(F32)
            up = along(low.astype(BF), range(0, step), 1)
            down = along(high.astype(BF), range(line_n - step, line_n), -1)
        return grads[:size] + up.astype(F32) + down.astype(F32)

    def finish_grad(accum, grads):
        total = line_sum(grads)
        mine = total[:depth]
        other = to_side(total[depth:].astype(BF)).astype(F32)
        return accum + jnp.where(
            side == 0,
            jnp.concatenate((mine, other), axis=1),
            jnp.concatenate((other, mine), axis=1),
        )

    order = [lax.rem(line - k + line_n, line_n) * 2 + (side ^ j) for k in range(line_n) for j in range(2)]
    core = tp % 2

    def both_sides(rows):
        piece = row_count // 2
        near = to_side(lax.dynamic_slice_in_dim(rows, core * piece, piece, 0))
        far = to_tp(near, 1)
        rows = jnp.concatenate(
            (rows, jnp.where(core == 0, near, far), jnp.where(core == 0, far, near)), axis=0
        )
        return jnp.concatenate(
            [lax.dynamic_slice_in_dim(rows, o * depth, depth, 1) for o in order], axis=1
        )

    def share_out(term):
        value = term.astype(BF)
        bit = 1
        outer = 2 * tp_n
        rest = row_count // tp_n
        value = value.reshape(2 * tp_n, rest, width)
        while bit < tp_n:
            outer //= 2
            view = value.reshape(outer, 2, rest, width)
            mine = (tp // bit) % 2
            keep = lax.dynamic_index_in_dim(view, mine, 1, keepdims=False)
            send = lax.dynamic_index_in_dim(view, 1 - mine, 1, keepdims=False)
            value = (keep.astype(F32) + to_tp(send, bit).astype(F32)).astype(BF)
            bit *= 2
        blocks = [
            lax.dynamic_slice_in_dim(
                value, (lax.rem(line - b // 2 + line_n, line_n) * 2 + (side ^ (b % 2))) * depth, depth, 2
            )
            for b in range(fs_n)
        ]
        value = jnp.concatenate(blocks, axis=2)
        return (value[0].astype(F32) + to_side(value[1]).astype(F32)).astype(BF)

    up_block = side_block(proj_up)
    saved_all = both_sides(saved_rows)
    upstream_all = both_sides(upstream_grad)
    fresh_all = both_sides(fresh_rows)
    up_whole, last = line_gather(up_block)
    down_block = side_block(proj_down)
    down_block, _ = lax.optimization_barrier((down_block, last))
    down_whole, _ = line_gather(down_block)

    saved_pre = jnp.dot(saved_all, up_whole, preferred_element_type=F32)
    saved_active, saved_hidden = squared_relu(saved_pre)
    accum_down_out = finish_grad(
        accum_down, grad_scale * over_tokens(upstream_all, saved_hidden)
    )
    fresh_hidden = squared_relu(jnp.dot(fresh_all, up_whole, preferred_element_type=F32))[1]
    hidden_grad = jnp.dot(upstream_all, down_whole, preferred_element_type=F32)
    pre_grad = (2.0 * saved_active * hidden_grad).astype(BF)
    accum_up_out = finish_grad(accum_up, grad_scale * over_tokens(saved_all, pre_grad))
    fresh_out = share_out(against_rows(fresh_hidden, down_whole))
    saved_grad = share_out(against_rows(pre_grad, up_whole))
    return (fresh_out, saved_grad, accum_up_out, accum_down_out)


def solution(mesh):
    in_specs = (P("fs", None),) * 3 + (P("fs", "tp"),) * 4
    out_specs = (P(("fs", "tp"), None),) * 2 + (P("fs", "tp"),) * 2
    return jax.shard_map(body, mesh=mesh, in_specs=in_specs, out_specs=out_specs, check_vma=False)
```

```python
import jax
import jax.numpy as jnp
from jax import lax
from jax.sharding import PartitionSpec as P


BF = jnp.bfloat16
F32 = jnp.float32


def against_rows(left, right):
    return lax.dot_general(left, right, (((1,), (1,)), ((), ())), preferred_element_type=F32)


def over_tokens(left, right):
    return lax.dot_general(left, right, (((0,), (0,)), ((), ())), preferred_element_type=F32)


def squared_relu(pre_values):
    active = jnp.maximum(pre_values, 0.0)
    return (active, (active * active).astype(BF))


def after(value, *earlier):
    return lax.optimization_barrier((value, earlier))[0]


def body(fresh_rows, saved_rows, upstream_grad, proj_up, proj_down, accum_up, accum_down):
    fs_n, tp_n = lax.axis_size("fs"), lax.axis_size("tp")
    line_n = fs_n // 2
    fs, tp = lax.axis_index("fs"), lax.axis_index("tp")
    line, side = fs // 2, fs % 2
    row_count, width = fresh_rows.shape
    depth, columns = proj_up.shape
    half = columns // 2
    grad_scale = float(row_count * fs_n) ** (-0.5)

    def to_side(value):
        return lax.ppermute(value, "fs", [(i, i ^ 1) for i in range(fs_n)])

    def to_tp(value, bit):
        return lax.ppermute(value, "tp", [(j, j ^ bit) for j in range(tp_n)])

    def along(value, lines, way):
        return lax.ppermute(
            value,
            "fs",
            [(l * 2 + s, (l + way) * 2 + s) for l in lines for s in range(2)],
        )

    def side_block(weight):
        mine = lax.dynamic_slice_in_dim(weight, side * half, half, 1)
        other = lax.dynamic_slice_in_dim(weight, (1 - side) * half, half, 1)
        return mine, to_side(other)

    def line_gather(block, ties={}):
        ups, downs = [block], [block]
        for step in range(1, line_n):
            up, down = after((ups[-1], downs[-1]), *ties.get(step, ()))
            up = along(up, range(step - 1, line_n - 1), 1)
            down = along(down, range(1, line_n - step + 1), -1)
            up, down = lax.optimization_barrier((up, down))
            ups.append(up)
            downs.append(down)
        blocks = [block] + [
            jnp.where(line >= k, ups[k], downs[line_n - k]) for k in range(1, line_n)
        ]
        return jnp.concatenate(blocks, axis=0), ups

    def line_sum(grads, ties={}):
        size = 2 * depth
        up = down = None
        marks = []
        for step in range(1, line_n):
            low = grads[step * size : (step + 1) * size]
            high = grads[(line_n - step) * size : (line_n - step + 1) * size]
            low = low if up is None else low + up.astype(F32)
            high = high if down is None else high + down.astype(F32)
            low, high = after((low.astype(BF), high.astype(BF)), *ties.get(step, ()))
            up = along(low, range(0, step), 1)
            down = along(high, range(line_n - step, line_n), -1)
            up, down = lax.optimization_barrier((up, down))
            marks.append(up)
        return grads[:size] + up.astype(F32) + down.astype(F32), marks

    def finish_grad(accum, total, other):
        mine = total[:depth]
        other = other.astype(F32)
        return accum + jnp.where(
            side == 0,
            jnp.concatenate((mine, other), axis=1),
            jnp.concatenate((other, mine), axis=1),
        )

    order = [lax.rem(line - k + line_n, line_n) * 2 + (side ^ j) for k in range(line_n) for j in range(2)]
    core = tp % 2

    def near_rows(rows):
        piece = row_count // 2
        return to_side(lax.dynamic_slice_in_dim(rows, core * piece, piece, 0))

    def both_sides(rows, near):
        far = to_tp(near, 1)
        rows = jnp.concatenate(
            (rows, jnp.where(core == 0, near, far), jnp.where(core == 0, far, near)), axis=0
        )
        return jnp.concatenate(
            [lax.dynamic_slice_in_dim(rows, o * depth, depth, 1) for o in order], axis=1
        )

    def share_tp(term):
        value = term.astype(BF)
        bit, stages = 1, []
        outer = 2 * tp_n
        rest = row_count // tp_n
        value = value.reshape(2 * tp_n, rest, width)
        while bit < tp_n:
            outer //= 2
            view = value.reshape(outer, 2, rest, width)
            mine = (tp // bit) % 2
            keep = lax.dynamic_index_in_dim(view, mine, 1, keepdims=False)
            send = lax.dynamic_index_in_dim(view, 1 - mine, 1, keepdims=False)
            value = (keep.astype(F32) + to_tp(send, bit).astype(F32)).astype(BF)
            bit *= 2
            stages.append(value)
        return stages

    def share_side(value):
        blocks = [
            lax.dynamic_slice_in_dim(
                value, (lax.rem(line - b // 2 + line_n, line_n) * 2 + (side ^ (b % 2))) * depth, depth, 2
            )
            for b in range(fs_n)
        ]
        value = jnp.concatenate(blocks, axis=2)
        return (value[0].astype(F32) + to_side(value[1]).astype(F32)).astype(BF)

    up_pair = side_block(proj_up)
    down_pair = side_block(proj_down)
    rows = after((saved_rows, upstream_grad, fresh_rows), down_pair[1])
    nears = [near_rows(r) for r in rows]
    up_whole, ups = line_gather(jnp.concatenate(up_pair, axis=0))
    saved_all = both_sides(rows[0], after(nears[0], ups[max(line_n - 2, 1)]))
    upstream_all = both_sides(rows[1], after(nears[1], ups[-1]))
    down_start = after(jnp.concatenate(down_pair, axis=0), ups[-1])
    saved_pre = jnp.dot(saved_all, up_whole, preferred_element_type=F32)
    saved_active, saved_hidden = squared_relu(saved_pre)
    down_grads = grad_scale * over_tokens(upstream_all, saved_hidden)
    down_total, _ = line_sum(down_grads)
    fresh_all = both_sides(rows[2], after(nears[2], down_grads))
    fresh_hidden = squared_relu(jnp.dot(fresh_all, up_whole, preferred_element_type=F32))[1]
    down_whole, _ = line_gather(down_start, {2: (down_grads,), 3: (fresh_hidden,)})
    hidden_grad = jnp.dot(upstream_all, down_whole, preferred_element_type=F32)
    pre_grad = (2.0 * saved_active * hidden_grad).astype(BF)
    up_grads = grad_scale * over_tokens(saved_all, pre_grad)
    fresh_hidden, pre_grad, _ = lax.optimization_barrier((fresh_hidden, pre_grad, up_grads))
    fresh_stages = share_tp(against_rows(fresh_hidden, down_whole))
    saved_stages = share_tp(against_rows(pre_grad, up_whole))
    up_total, marks = line_sum(
        up_grads, {2: (fresh_stages[0], saved_stages[0]), 3: (fresh_stages[-1],)}
    )
    middle = marks[max(line_n - 3, 0)]
    fresh_out = share_side(fresh_stages[-1])
    saved_grad = share_side(saved_stages[-1])
    down_other = after(to_side(down_total[depth:].astype(BF)), middle)
    accum_down_out = finish_grad(accum_down, down_total, down_other)
    accum_up_out = finish_grad(accum_up, up_total, to_side(up_total[depth:].astype(BF)))
    return (fresh_out, saved_grad, accum_up_out, accum_down_out)


def solution(mesh):
    in_specs = (P("fs", None),) * 3 + (P("fs", "tp"),) * 4
    out_specs = (P(("fs", "tp"), None),) * 2 + (P("fs", "tp"),) * 2
    return jax.shard_map(body, mesh=mesh, in_specs=in_specs, out_specs=out_specs, check_vma=False)
```
